32 devices in a mesh: ep: 16 (over z, y, x), tp: 2 (over core).
Axes of the slice: x: 2, y: 2, z: 4, core: 2. Of those that a mesh axis runs over, the one named last changes fastest.
Arguments:
- tokens: bfloat16 [16, 2048], P('ep'), may hold values from -6 to 6
- norm_gain: float32 [2048], replicated, may hold values from 0.1 to 1.9
- w_query: bfloat16 [2048, 512], P('ep', 'tp'), may hold values from -0.125 to 0.125
- w_key: bfloat16 [2048, 512], P('ep', 'tp'), may hold values from -0.125 to 0.125
- w_value: bfloat16 [2048, 1024], P('ep', 'tp'), may hold values from -0.125 to 0.125
- w_outgate: bfloat16 [2048, 1024], P('ep', 'tp'), may hold values from -0.125 to 0.125
- decay_in: bfloat16 [2048, 16], replicated, may hold values from -0.125 to 0.125
- decay_out: bfloat16 [16, 512], P(None, 'tp'), may hold values from -1.5 to 1.5
- decay_bias: float32 [512], P('tp'), may hold values from -40 to 4
- gla_state: float32 [16, 2, 256, 512], P('ep', 'tp'), may hold values from -6 to 6
- head_gain: float32 [512], replicated, may hold values from 0.1 to 1.9
- w_output: bfloat16 [1024, 2048], P(None, 'ep'), may hold values from -0.1875 to 0.1875
- moe_gain: float32 [2048], replicated, may hold values from 0.1 to 1.9
- expert_ids: int32 [16, 6], replicated, may hold values from 0 to 15, all different within a row; in each aligned block of 16 rows (0 to 15, 16 to 31, ...) at most 12 rows name the same one
- route_weight: float32 [16, 6], replicated, may hold values from 0.2 to 1
- expert_gate: bfloat16 [16, 2048, 512], P('ep', None, 'tp'), may hold values from -0.125 to 0.125
- expert_up: bfloat16 [16, 2048, 512], P('ep', None, 'tp'), may hold values from -0.125 to 0.125
- expert_down: bfloat16 [16, 512, 2048], P('ep', 'tp'), may hold values from -0.25 to 0.25
- shared_gate: bfloat16 [2048, 512], P(None, 'tp'), may hold values from -0.125 to 0.125
- shared_up: bfloat16 [2048, 512], P(None, 'tp'), may hold values from -0.125 to 0.125
- shared_down: bfloat16 [512, 2048], P('tp'), may hold values from -0.25 to 0.25
Outputs:
- result: bfloat16 [16, 2048], P(None, 'ep')
- new_state: float32 [16, 2, 256, 512], P('ep', 'tp')
The draws below stay inside these ranges and needn't reach their ends.
Inputs may be any that keep to these rules, and one draw needn't show every extreme that they name: `expert_ids`: each row names 6 different experts. No expert is named by more than 12 rows in all, a bound that some block reaches.
All inputs are finite; a program needn't handle non-finite values.
Results may differ from the reference program's by a relative error of at most 0.018.
Values may be sent and summed in bfloat16 or wider, within the bound.
No kernel may reach another device: no remote copies, remote signals or barrier semaphores. Data moves between devices by JAX's collectives and lax.ppermute only.
A program may use at most 64 MiB of HBM per device.

```python
import math
import jax
import jax.numpy as jnp
import numpy as np
from jax import lax

D = 2048
HEADS = 2
DK = 256
DV = 512
RANK = 16
F = 512
TOP = 6
TOKENS = 16
EXPERTS = 16
CAP = 12
N_TP = 2


def spiked(values, rng, source, target, parts, factor):
    owner, partner = [(jnp.arange(values.shape[dim]) // (values.shape[dim] // parts)).reshape([-1 if axis == dim else 1 for axis in range(values.ndim)]) for dim in (source, target)]
    chosen = jax.random.permutation(rng, parts)[partner]
    strong = (owner == chosen) | (owner == (partner + parts // 2) % parts)
    return jnp.where(strong, factor * values, values)


def block_levels(own_key, dims, shards, least, high):
    loudness = 1.0
    for dim, shards_of in shards:
        steps = jax.random.uniform(jax.random.fold_in(jax.random.fold_in(own_key, 6), dim), (shards_of,), jnp.float32, least / len(shards), high / len(shards))
        loudness = loudness * jnp.repeat(jnp.exp(steps), dims[dim] // shards_of).reshape((-1,) + (1,) * (len(dims) - 1 - dim))
    return loudness


def deal_out(own_key, own, number, rows, amount, top, most, lean):
    order = jax.random.permutation(own_key, amount)
    packed, usual = load_shares(amount, rows * top, most, lean, True), load_shares(amount, rows * top, most, lean, False)
    places = jnp.arange(amount)

    def named(lengths, turn):
        used = int((lengths > 0).sum())
        fixed = max(1, used // 4)
        passed = fixed + (places - fixed + turn * (used - fixed)) % max(1, amount - fixed)
        return jnp.zeros((amount,), jnp.int32).at[order[jnp.where(places < fixed, places, passed)]].set(jnp.asarray(lengths, jnp.int32))

    lengths = jnp.where(number % 4 == 0, named(packed, number // 4), named(usual, number - number // 4 - 1))
    mixed = jax.random.permutation(jax.random.fold_in(own, 3), amount)
    source_of, taker = mixed[0:amount // 2 * 2:2], mixed[1:amount // 2 * 2:2]
    slack = jnp.minimum(lengths[source_of] - 1, most - lengths[taker]) // 2
    slack = jnp.where((source_of == order[0]) | (taker == order[0]) | (lengths[taker] == 0), 0, jnp.maximum(slack, 0))
    passed = jax.random.randint(jax.random.fold_in(own, 4), (amount // 2,), 0, 1 << 20) % (slack + 1)
    lengths = lengths.at[source_of].add(-passed).at[taker].add(passed)
    items = jnp.searchsorted(jnp.cumsum(lengths), jnp.arange(rows * top), side="right").astype(jnp.int32)
    grid = items.reshape(top, rows).T
    grid = grid[jax.random.permutation(jax.random.fold_in(own, 1), rows)]
    turn = jax.random.randint(jax.random.fold_in(own, 2), (rows, 1), 0, top)
    return jnp.take_along_axis(grid, (jnp.arange(top)[None, :] + turn) % top, axis=1)


def load_shares(count, total, limit, lean, full):
    portions = [(1 << 20) // math.isqrt(standing ** lean) + 1 for standing in range(1, count + 1)]
    largest = limit if full else min(limit, max(-(-total // count), total * portions[0] // sum(portions)))
    least = 1 if total - largest >= count - 1 else 0
    counts, spare = [largest] + [least] * (count - 1), total - largest - least * (count - 1)
    while spare > 0:
        candidates = [i for i in range(1, count) if counts[i] < largest] or [i for i in range(1, count) if counts[i] < limit]
        pool, remaining = sum([portions[i] for i in candidates]), spare
        for i in candidates:
            addition = min(limit - counts[i], max(1, remaining * portions[i] // pool), spare)
            counts[i] = counts[i] + addition
            spare = spare - addition
    return np.array(counts)


def noise(stream_key, dims, scale, reach, cuts=(), kind=jnp.bfloat16):
    array = jax.random.normal(stream_key, dims, jnp.float32) * scale
    if len(cuts) > 0:
        array = block_levels(stream_key, dims, cuts, -0.22, 0.18) * array
    return jnp.clip(array, min=-reach, max=reach).astype(kind)


def heavy_noise(key, extent, scale, limit, shards, heavy, kind=jnp.bfloat16):
    values = scale * jax.random.normal(key, extent, jnp.float32)
    if shards:
        values = values * block_levels(key, extent, shards, -0.22, 0.18)
    return jnp.clip(spiked(values, jax.random.fold_in(key, 3), *heavy), -limit, limit).astype(kind)


def setup_inputs(seed: int = 0) -> dict:
    key_list = jax.random.split(jax.random.key(seed), 22)
    tokens = heavy_noise(key_list[0], (TOKENS, D), 1.0, 6.0, ((0, 16),), (1, 0, 16, 2.0))
    norm_gain = jnp.clip(1.0 + 0.18 * jax.random.normal(key_list[1], (D,), jnp.float32), 0.1, 1.9)
    w_query = noise(key_list[2], (D, HEADS * DK), D ** -0.5, 0.125, ((0, 16), (1, 2)))
    w_key = noise(key_list[3], (D, HEADS * DK), D ** -0.5, 0.125, ((0, 16), (1, 2)))
    w_value = noise(key_list[4], (D, HEADS * DV), D ** -0.5, 0.125, ((0, 16), (1, 2)))
    w_outgate = noise(key_list[5], (D, HEADS * DV), D ** -0.5, 0.125, ((0, 16), (1, 2)))
    decay_in = noise(key_list[6], (D, RANK), D ** -0.5, 0.125)
    decay_out = noise(key_list[7], (RANK, HEADS * DK), RANK ** -0.5, 1.5, ((1, 2),))
    decay_bias = jnp.clip(-40.0 + 44.0 * jax.random.uniform(key_list[8], (HEADS * DK,), jnp.float32) ** block_levels(key_list[8], (HEADS * DK,), ((0, 2),), -0.2, 0.2), -40.0, 4.0)
    gla_state = noise(key_list[9], (TOKENS, HEADS, DK, DV), 1.0, 6.0, ((0, 16), (1, 2)), jnp.float32)
    head_gain = jnp.clip(1.0 + 0.18 * jax.random.normal(key_list[10], (DV,), jnp.float32), 0.1, 1.9)
    w_output = noise(key_list[11], (HEADS * DV, D), (HEADS * DV) ** -0.5, 0.1875, ((1, 16),))
    moe_gain = jnp.clip(1.0 + 0.18 * jax.random.normal(key_list[12], (D,), jnp.float32), 0.1, 1.9)
    expert_ids_keys = jax.random.split(jax.random.fold_in(key_list[13], 1), TOKENS // TOKENS)
    expert_ids_turns = jax.random.permutation(jax.random.fold_in(key_list[13], 3), TOKENS // TOKENS)
    expert_ids = jax.vmap(lambda own, number: deal_out(jax.random.fold_in(key_list[13], 2), own, number, TOKENS, EXPERTS, TOP, CAP, 2))(expert_ids_keys, expert_ids_turns).reshape((TOKENS, TOP))
    route_weight = jnp.clip(jax.random.uniform(key_list[14], (TOKENS, TOP), jnp.float32, 0.2, 1.0), 0.2, 1.0)
    expert_gate = noise(key_list[15], (EXPERTS, D, F), D ** -0.5, 0.125, ((0, 16), (2, 2)))
    expert_up = noise(key_list[16], (EXPERTS, D, F), D ** -0.5, 0.125, ((0, 16), (2, 2)))
    expert_down = noise(key_list[17], (EXPERTS, F, D), F ** -0.5, 0.25, ((0, 16), (1, 2)))
    shared_gate = noise(key_list[18], (D, F), D ** -0.5, 0.125, ((1, 2),))
    shared_up = noise(key_list[19], (D, F), D ** -0.5, 0.125, ((1, 2),))
    shared_down = noise(key_list[20], (F, D), F ** -0.5, 0.25, ((0, 2),))
    return {"tokens": tokens, "norm_gain": norm_gain, "w_query": w_query, "w_key": w_key, "w_value": w_value, "w_outgate": w_outgate, "decay_in": decay_in, "decay_out": decay_out, "decay_bias": decay_bias, "gla_state": gla_state, "head_gain": head_gain, "w_output": w_output, "moe_gain": moe_gain, "expert_ids": expert_ids, "route_weight": route_weight, "expert_gate": expert_gate, "expert_up": expert_up, "expert_down": expert_down, "shared_gate": shared_gate, "shared_up": shared_up, "shared_down": shared_down}


EPSILON = 1e-06
DECAY_TEMPER = 16.0

def rms_scale(values):
    return lax.rsqrt(lax.optimization_barrier(jnp.mean(values * values, axis=-1, keepdims=True)) + EPSILON)

def slot_positions(expert_ids, expert_count):
    flat_ids = expert_ids.reshape(-1).astype(jnp.int32)
    onehot = (flat_ids[:, None] == jnp.arange(expert_count, dtype=jnp.int32)[None, :]).astype(jnp.int32)
    before = jnp.cumsum(onehot, axis=0) - onehot
    position = lax.optimization_barrier(jnp.sum(before * onehot, axis=1)).astype(jnp.int32)
    return (flat_ids, position)

def rounded_add(running, partial_sum):
    held = lax.optimization_barrier(partial_sum.astype(jnp.bfloat16))
    return running + held.astype(jnp.float32)

def swiglu_halves(rows, gate_weight, up_weight, down_weight, halves):
    half_width = gate_weight.shape[1] // halves
    running = jnp.zeros((rows.shape[0], down_weight.shape[1]), jnp.float32)
    for half_index in range(halves):
        lower_edge = half_index * half_width
        upper_edge = lower_edge + half_width
        gate_values = jnp.dot(rows, gate_weight[:, lower_edge:upper_edge], preferred_element_type=jnp.float32)
        upward = jnp.dot(rows, up_weight[:, lower_edge:upper_edge], preferred_element_type=jnp.float32)
        active = (jax.nn.silu(gate_values) * upward).astype(jnp.bfloat16)
        running = rounded_add(running, jnp.dot(active, down_weight[lower_edge:upper_edge], preferred_element_type=jnp.float32))
    return running.astype(jnp.bfloat16)

def reference(tokens, norm_gain, w_query, w_key, w_value, w_outgate, decay_in, decay_out, decay_bias, gla_state, head_gain, w_output, moe_gain, expert_ids, route_weight, expert_gate, expert_up, expert_down, shared_gate, shared_up, shared_down):
    seq_count = tokens.shape[0]
    tok_float = tokens.astype(jnp.float32)
    normed = (tok_float * rms_scale(tok_float) * norm_gain).astype(jnp.bfloat16)
    query_rows = jnp.dot(normed, w_query, preferred_element_type=jnp.float32).astype(jnp.bfloat16)
    key_rows = jnp.dot(normed, w_key, preferred_element_type=jnp.float32).astype(jnp.bfloat16)
    value_rows = jnp.dot(normed, w_value, preferred_element_type=jnp.float32).astype(jnp.bfloat16)
    gate_rows = jnp.dot(normed, w_outgate, preferred_element_type=jnp.float32).astype(jnp.bfloat16)
    decay_low = jnp.dot(normed, decay_in, preferred_element_type=jnp.float32).astype(jnp.bfloat16)
    decay_pre = jnp.dot(decay_low, decay_out, preferred_element_type=jnp.float32) + decay_bias
    decay_rate = jnp.exp(jax.nn.log_sigmoid(decay_pre) / DECAY_TEMPER).reshape(seq_count, HEADS, DK)
    query_heads = query_rows.astype(jnp.float32).reshape(seq_count, HEADS, DK) * DK ** (-0.5)
    key_heads = key_rows.astype(jnp.float32).reshape(seq_count, HEADS, DK)
    value_heads = value_rows.astype(jnp.float32).reshape(seq_count, HEADS, DV)
    new_state = decay_rate[..., None] * gla_state + key_heads[..., None] * value_heads[:, :, None, :]
    read_out = jnp.einsum('shk,shkv->shv', query_heads, new_state, precision=lax.Precision.HIGHEST)
    gate_heads = gate_rows.astype(jnp.float32).reshape(seq_count, HEADS, DV)
    mixed_heads = (read_out * rms_scale(read_out) * head_gain * jax.nn.silu(gate_heads)).astype(jnp.bfloat16)
    mixed_heads = mixed_heads.reshape(seq_count, HEADS * DV)
    attention = jnp.dot(mixed_heads, w_output, preferred_element_type=jnp.float32).astype(jnp.bfloat16)
    hidden = (tok_float + attention.astype(jnp.float32)).astype(jnp.bfloat16)
    hid_float = hidden.astype(jnp.float32)
    hnorm = (hid_float * rms_scale(hid_float) * moe_gain).astype(jnp.bfloat16)
    flat_ids, position = slot_positions(expert_ids, EXPERTS)
    owner_rows = jnp.arange(seq_count * TOP, dtype=jnp.int32) // TOP
    slot_table = jnp.full((EXPERTS, CAP), seq_count, jnp.int32).at[flat_ids, position].set(owner_rows)
    padded = jnp.concatenate([hnorm, jnp.zeros((1, D), jnp.bfloat16)], axis=0)

    def one_expert(operands):
        index_rows, gate_weight, up_weight, down_weight = operands
        return swiglu_halves(padded[index_rows], gate_weight, up_weight, down_weight, N_TP)
    expert_out = lax.map(one_expert, (slot_table, expert_gate, expert_up, expert_down))
    picked = expert_out.reshape(EXPERTS * CAP, D)[(flat_ids * CAP + position).astype(jnp.int32)]
    routed = lax.optimization_barrier(jnp.sum(picked.astype(jnp.float32).reshape(seq_count, TOP, D) * route_weight[..., None], axis=1))
    shared_out = swiglu_halves(hnorm, shared_gate, shared_up, shared_down, N_TP)
    result = (hid_float + routed + shared_out.astype(jnp.float32)).astype(jnp.bfloat16)
    return (result, new_state)
```

```python
import jax
import jax.numpy as jnp
from jax import lax
from jax.sharding import PartitionSpec as P

EPSILON = 1e-06
DECAY_TEMPER = 16.0
LANES = 128
F32 = jnp.float32
BF16 = jnp.bfloat16


def rms_scale(values):
    return lax.rsqrt(jnp.mean(values * values, axis=-1, keepdims=True) + EPSILON)


def exchange(blocks, axes):
    return lax.all_to_all(blocks, axes, split_axis=0, concat_axis=0, tiled=True)


def tp_sum(values):
    tp_size = lax.axis_size("tp")
    both = lax.all_gather(values, "tp", axis=0, tiled=False)
    total = both[0]
    for member in range(1, tp_size):
        total = total + both[member]
    return total


def per_device(
    tokens,
    norm_gain,
    w_query,
    w_key,
    w_value,
    w_outgate,
    decay_in,
    decay_out,
    decay_bias,
    gla_state,
    head_gain,
    w_output,
    moe_gain,
    expert_ids,
    route_weight,
    expert_gate,
    expert_up,
    expert_down,
    shared_gate,
    shared_up,
    shared_down,
):
    ep_size = lax.axis_size("ep")
    tp_size = lax.axis_size("tp")
    ep_index = lax.axis_index("ep")
    seq_dev, width = tokens.shape
    exp_dev = expert_gate.shape[0]
    all_rows = seq_dev * ep_size
    block = width // ep_size
    dk, dv = gla_state.shape[2:]
    heads_local = gla_state.shape[1]
    tok_float = tokens.astype(F32)
    normed = (tok_float * rms_scale(tok_float) * norm_gain).astype(BF16)
    outgoing = jnp.concatenate(
        [tokens.reshape(seq_dev, ep_size, block), normed.reshape(seq_dev, ep_size, block)], axis=0
    ).transpose(1, 0, 2)
    columns = exchange(outgoing, "ep")
    raw_columns = columns[:, :seq_dev].reshape(all_rows, block)
    normed_columns = columns[:, seq_dev:].reshape(all_rows, block)
    weights = (w_query, w_key, w_value, w_outgate)
    partial = jnp.concatenate(
        [jnp.dot(normed_columns, w, preferred_element_type=F32).astype(BF16) for w in weights],
        axis=1,
    )
    spans = partial.shape[1]
    partial = partial.reshape(ep_size, seq_dev * spans // LANES, LANES)
    joined = jnp.sum(exchange(partial, "ep").astype(F32), axis=0).reshape(seq_dev, spans)
    joined = joined.astype(BF16).astype(F32)
    edges = [0]
    for w in weights:
        edges.append(edges[-1] + w.shape[1])
    query, key, value, gate = (joined[:, edges[n] : edges[n + 1]] for n in range(4))
    decay_low = jnp.dot(normed, decay_in, preferred_element_type=F32).astype(BF16)
    decay_pre = jnp.dot(decay_low, decay_out, preferred_element_type=F32) + decay_bias
    decay_rate = jnp.exp(jax.nn.log_sigmoid(decay_pre) / DECAY_TEMPER)
    decay_rate = decay_rate.reshape(seq_dev, heads_local, dk)
    query = query.reshape(seq_dev, heads_local, dk) * dk ** (-0.5)
    key = key.reshape(seq_dev, heads_local, dk)
    value = value.reshape(seq_dev, heads_local, dv)
    gate = gate.reshape(seq_dev, heads_local, dv)
    new_state = decay_rate[..., None] * gla_state + key[..., None] * value[:, :, None, :]
    read_out = jnp.sum(query[..., None] * new_state, axis=2)
    mixed = (read_out * rms_scale(read_out) * head_gain * jax.nn.silu(gate)).astype(BF16)
    mixed = mixed.reshape(1, seq_dev * heads_local * dv // LANES, LANES)
    spread = exchange(
        jnp.broadcast_to(mixed, (ep_size * tp_size,) + mixed.shape[1:]), ("ep", "tp")
    )
    heads = spread.reshape(ep_size, tp_size, seq_dev, heads_local * dv)
    heads = heads.transpose(0, 2, 1, 3).reshape(all_rows, tp_size * heads_local * dv)
    attention = jnp.dot(heads, w_output, preferred_element_type=F32).astype(BF16)
    hidden = (raw_columns.astype(F32) + attention.astype(F32)).astype(BF16)
    rows = exchange(jnp.broadcast_to(hidden[None], (ep_size,) + hidden.shape), "ep")
    rows = rows.transpose(1, 0, 2).reshape(all_rows, width)
    row_float = rows.astype(F32)
    normal_rows = (row_float * rms_scale(row_float) * moe_gain).astype(BF16)
    routed = jnp.zeros((all_rows, width), F32)
    for number in range(exp_dev):
        expert = ep_index * exp_dev + number
        share = jnp.sum(jnp.where(expert_ids == expert, route_weight, 0.0), axis=1, keepdims=True)
        gate_values = jnp.dot(normal_rows, expert_gate[number], preferred_element_type=F32)
        upward = jnp.dot(normal_rows, expert_up[number], preferred_element_type=F32)
        active = (jax.nn.silu(gate_values) * upward).astype(BF16)
        routed = routed + share * jnp.dot(
            active, expert_down[number], preferred_element_type=F32
        )
    outgoing = routed.astype(BF16).reshape(all_rows, ep_size, block).transpose(1, 0, 2)
    back = exchange(outgoing, "ep")
    shared_values = jnp.dot(normal_rows, shared_gate, preferred_element_type=F32)
    shared_upward = jnp.dot(normal_rows, shared_up, preferred_element_type=F32)
    shared_active = (jax.nn.silu(shared_values) * shared_upward).astype(BF16)
    down_columns = lax.dynamic_slice_in_dim(shared_down, ep_index * block, block, 1)
    shared_part = jnp.dot(shared_active, down_columns, preferred_element_type=F32)
    moe_columns = tp_sum(shared_part + jnp.sum(back.astype(F32), axis=0))
    result = (hidden.astype(F32) + moe_columns).astype(BF16)
    return (result, new_state)


def solution(mesh):
    return jax.shard_map(
        per_device,
        mesh=mesh,
        in_specs=(
            P("ep", None),
            P(),
            P("ep", "tp"),
            P("ep", "tp"),
            P("ep", "tp"),
            P("ep", "tp"),
            P(),
            P(None, "tp"),
            P("tp"),
            P("ep", "tp", None, None),
            P(),
            P(None, "ep"),
            P(),
            P(),
            P(),
            P("ep", None, "tp"),
            P("ep", None, "tp"),
            P("ep", "tp", None),
            P(None, "tp"),
            P(None, "tp"),
            P("tp", None),
        ),
        out_specs=(P(None, "ep"), P("ep", "tp", None, None)),
        check_vma=False,
    )
```

```python
import jax
import jax.numpy as jnp
from jax import lax
from jax.sharding import PartitionSpec as P

EPSILON = 1e-06
DECAY_TEMPER = 16.0
LANES = 128
F32 = jnp.float32
BF16 = jnp.bfloat16


def rms_scale(values):
    return lax.rsqrt(jnp.mean(values * values, axis=-1, keepdims=True) + EPSILON)


def exchange(blocks, axes):
    return lax.all_to_all(blocks, axes, split_axis=0, concat_axis=0, tiled=True)


def tp_sum(values):
    tp_size = lax.axis_size("tp")
    both = lax.all_gather(values, "tp", axis=0, tiled=False)
    total = both[0]
    for member in range(1, tp_size):
        total = total + both[member]
    return total


def per_device(
    tokens,
    norm_gain,
    w_query,
    w_key,
    w_value,
    w_outgate,
    decay_in,
    decay_out,
    decay_bias,
    gla_state,
    head_gain,
    w_output,
    moe_gain,
    expert_ids,
    route_weight,
    expert_gate,
    expert_up,
    expert_down,
    shared_gate,
    shared_up,
    shared_down,
):
    ep_size = lax.axis_size("ep")
    tp_size = lax.axis_size("tp")
    ep_index = lax.axis_index("ep")
    seq_dev, width = tokens.shape
    exp_dev = expert_gate.shape[0]
    all_rows = seq_dev * ep_size
    block = width // ep_size
    dk, dv = gla_state.shape[2:]
    heads_local = gla_state.shape[1]
    everywhere = ("ep", "tp")
    outgoing = tokens.reshape(seq_dev, ep_size, 1, block).transpose(1, 2, 0, 3)
    outgoing = jnp.broadcast_to(outgoing, (ep_size, tp_size, seq_dev, block))
    columns = exchange(outgoing.reshape(ep_size * tp_size, seq_dev, block), everywhere)
    raw_columns = columns.reshape(ep_size, tp_size, seq_dev, block)[:, 0].reshape(all_rows, block)
    gain_block = lax.dynamic_slice_in_dim(norm_gain, ep_index * block, block, 0)
    gained_columns = (raw_columns.astype(F32) * gain_block).astype(BF16)
    tok_float = tokens.astype(F32)
    tok_scale = rms_scale(tok_float)
    normed = (tok_float * tok_scale * norm_gain).astype(BF16)
    weights = (w_query, w_key, w_value, w_outgate)
    partial = jnp.concatenate(
        [jnp.dot(gained_columns, w, preferred_element_type=F32).astype(BF16) for w in weights],
        axis=1,
    )
    spans = partial.shape[1]
    partial = partial.reshape(ep_size, seq_dev * spans // LANES, LANES)
    joined = jnp.sum(exchange(partial, "ep").astype(F32), axis=0).reshape(seq_dev, spans)
    joined = (joined * tok_scale).astype(BF16).astype(F32)
    edges = [0]
    for w in weights:
        edges.append(edges[-1] + w.shape[1])
    query, key, value, gate = (joined[:, edges[n] : edges[n + 1]] for n in range(4))
    decay_low = jnp.dot(normed, decay_in, preferred_element_type=F32).astype(BF16)
    decay_pre = jnp.dot(decay_low, decay_out, preferred_element_type=F32) + decay_bias
    decay_rate = jnp.exp(jax.nn.log_sigmoid(decay_pre) / DECAY_TEMPER)
    decay_rate = decay_rate.reshape(seq_dev, heads_local, dk)
    query = query.reshape(seq_dev, heads_local, dk) * dk ** (-0.5)
    key = key.reshape(seq_dev, heads_local, dk)
    value = value.reshape(seq_dev, heads_local, dv)
    gate = gate.reshape(seq_dev, heads_local, dv)
    new_state = decay_rate[..., None] * gla_state + key[..., None] * value[:, :, None, :]
    read_out = jnp.sum(query[..., None] * new_state, axis=2)
    mixed = (read_out * rms_scale(read_out) * head_gain * jax.nn.silu(gate)).astype(BF16)
    mixed = mixed.reshape(1, seq_dev * heads_local * dv // LANES, LANES)
    spread = exchange(
        jnp.broadcast_to(mixed, (ep_size * tp_size,) + mixed.shape[1:]), ("ep", "tp")
    )
    heads = spread.reshape(ep_size, tp_size, seq_dev, heads_local * dv)
    heads = heads.transpose(0, 2, 1, 3).reshape(all_rows, tp_size * heads_local * dv)
    attention = jnp.dot(heads, w_output, preferred_element_type=F32).astype(BF16)
    hidden = (raw_columns.astype(F32) + attention.astype(F32)).astype(BF16)
    part_rows = all_rows // tp_size
    own_rows = lax.dynamic_slice_in_dim(hidden, lax.axis_index("tp") * part_rows, part_rows, 0)
    rows = exchange(
        jnp.broadcast_to(own_rows[None], (ep_size * tp_size,) + own_rows.shape), everywhere
    )
    rows = rows.reshape(ep_size, tp_size, part_rows, block).transpose(1, 2, 0, 3)
    rows = rows.reshape(all_rows, width)
    row_float = rows.astype(F32)
    normal_rows = (row_float * rms_scale(row_float) * moe_gain).astype(BF16)
    routed = jnp.zeros((all_rows, width), F32)
    for number in range(exp_dev):
        expert = ep_index * exp_dev + number
        share = jnp.sum(jnp.where(expert_ids == expert, route_weight, 0.0), axis=1, keepdims=True)
        gate_values = jnp.dot(normal_rows, expert_gate[number], preferred_element_type=F32)
        upward = jnp.dot(normal_rows, expert_up[number], preferred_element_type=F32)
        active = (jax.nn.silu(gate_values) * upward).astype(BF16)
        routed = routed + share * jnp.dot(
            active, expert_down[number], preferred_element_type=F32
        )
    outgoing = routed.astype(BF16).reshape(all_rows, ep_size, 1, block).transpose(1, 2, 0, 3)
    outgoing = jnp.broadcast_to(outgoing, (ep_size, tp_size, all_rows, block))
    back = exchange(outgoing.reshape(ep_size * tp_size, all_rows, block), everywhere)
    shared_values = jnp.dot(normal_rows, shared_gate, preferred_element_type=F32)
    shared_upward = jnp.dot(normal_rows, shared_up, preferred_element_type=F32)
    shared_active = (jax.nn.silu(shared_values) * shared_upward).astype(BF16)
    down_columns = lax.dynamic_slice_in_dim(shared_down, ep_index * block, block, 1)
    shared_part = jnp.dot(shared_active, down_columns, preferred_element_type=F32)
    moe_columns = tp_sum(shared_part) + jnp.sum(back.astype(F32), axis=0)
    result = (hidden.astype(F32) + moe_columns).astype(BF16)
    return (result, new_state)


def solution(mesh):
    return jax.shard_map(
        per_device,
        mesh=mesh,
        in_specs=(
            P("ep", None),
            P(),
            P("ep", "tp"),
            P("ep", "tp"),
            P("ep", "tp"),
            P("ep", "tp"),
            P(),
            P(None, "tp"),
            P("tp"),
            P("ep", "tp", None, None),
            P(),
            P(None, "ep"),
            P(),
            P(),
            P(),
            P("ep", None, "tp"),
            P("ep", None, "tp"),
            P("ep", "tp", None),
            P(None, "tp"),
            P(None, "tp"),
            P("tp", None),
        ),
        out_specs=(P(None, "ep"), P("ep", "tp", None, None)),
        check_vma=False,
    )
```
